32 devices in a mesh: ep: 16 (over z, x, core), tp: 2 (over y).
Axes of the slice: x: 2, y: 2, z: 4, core: 2. Of those that a mesh axis runs over, the one named last changes fastest.
Arguments:
- tokens: bfloat16 [768, 2048], P('ep', 'tp'), may hold values from -80 to 80
- pre_gain: float32 [2048], P('tp'), may hold values from 0.1 to 1.9
- post_gain: float32 [2048], P('tp'), may hold values from 0.1 to 1.9
- group_logits: float32 [768, 16], P('ep'), may hold values from -12 to 12
- expert_logits: float32 [768, 6], P('ep'), may hold values from -9 to 330
- route_group: int32 [768, 6], P('ep'), may hold values from 0 to 15, all different within a row; in each aligned block of 48 rows (0 to 47, 48 to 95, ...) at most 27 rows name the same one
- route_expert: int32 [768, 6], P('ep'), may hold values from 0 to 15
- gate_weight: bfloat16 [256, 2048, 256], P('ep', 'tp'), may hold values from -0.125 to 0.125
- up_weight: bfloat16 [256, 2048, 256], P('ep', 'tp'), may hold values from -0.125 to 0.125
- down_weight: bfloat16 [256, 256, 2048], P('ep', None, 'tp'), may hold values from -48 to 48
Outputs:
- layer_out: bfloat16 [768, 2048], P('ep', 'tp')
The draws below stay inside these ranges and needn't reach their ends.
Inputs may be any that keep to these rules, and one draw needn't show every extreme that they name: `route_group`: each row names 6 different groups. The rows of one index of ep name any one group at most 27 times, a bound that some block reaches.
All inputs are finite; a program needn't handle non-finite values.
Results may differ from the reference program's by a relative error of at most 0.024.
Values may be sent and summed in bfloat16 or wider, within the bound.
A program may use at most 64 MiB of HBM per device.

```python
import math
import jax
import jax.numpy as jnp
import numpy as np
from jax import lax

D = 2048
FF = 256
TOPK = 6
EXP_DEV = 16
TOK_DEV = 48
GROUPS = 16
EXPERTS = 256
TOKENS = 768
CAP = 27
N_TP = 2


def draw_tokens(key, part):
    first = jax.random.fold_in(key, 0)
    columns = jnp.arange(D, dtype=jnp.float32) / (D - 1)
    base = jnp.clip(jax.random.normal(first, (TOKENS, D), jnp.float32), -6.0, 6.0)
    values = base * jnp.exp(columns * math.log(6.0))
    return values.astype(jnp.bfloat16)


def draw_down_weight(key, part):
    first, second = jax.random.split(key, 2)
    columns = jnp.arange(D, dtype=jnp.float32) / (D - 1)
    base = jnp.clip(jax.random.normal(first, (EXPERTS, FF, D), jnp.float32), -6.0, 6.0)
    level = jax.random.uniform(second, (EXPERTS, 1, 1), jnp.float32, -2.0, 2.0)
    values = base * jnp.exp(columns * math.log(6.0)) * jnp.exp(level) / math.sqrt(FF)
    return values.astype(jnp.bfloat16)


def draw_expert_logits(key, part):
    first = jax.random.fold_in(key, 0)
    base = jnp.clip(1.5 * jax.random.normal(first, (TOKENS, TOPK), jnp.float32), -6.0, 6.0)
    values = base
    return values.astype(jnp.float32)


def with_ends(array, own_key, least, top_value):
    shape = array.shape
    index_at = [jax.random.randint(jax.random.fold_in(own_key, axis), (), 0, shape[axis]) for axis in range(len(shape))]
    array = array.at[tuple(index_at)].set(least)
    longest = shape.index(max(shape))
    index_at[longest] = (index_at[longest] + 1) % shape[longest]
    return array.at[tuple(index_at)].set(top_value)


def levels(own_key, shape, cuts, least, top_value):
    def one(position, blocks):
        heights = jax.random.uniform(jax.random.fold_in(jax.random.fold_in(own_key, 6), position), (blocks,), jnp.float32, least / len(cuts), top_value / len(cuts))
        return jnp.repeat(jnp.exp(heights), shape[position] // blocks).reshape((-1,) + (1,) * (len(shape) - position - 1))

    level = one(*cuts[0])
    for cut in cuts[1:]:
        level = level * one(*cut)
    return level


def routed_block(key, own, number, rows, count, top, reach, slope):
    sequence = jax.random.permutation(key, count)
    packed, usual = load_shares(count, rows * top, reach, slope, True), load_shares(count, rows * top, reach, slope, False)
    places = jnp.arange(count)

    def named(tallies, rotation):
        used = int((tallies > 0).sum())
        fixed = max(1, used // 4)
        shifted = fixed + (places - fixed + rotation * (used - fixed)) % max(1, count - fixed)
        return jnp.zeros((count,), jnp.int32).at[sequence[jnp.where(places < fixed, places, shifted)]].set(jnp.asarray(tallies, jnp.int32))

    tallies = jnp.where(number % 4 == 0, named(packed, number // 4), named(usual, number - number // 4 - 1))
    mixed = jax.random.permutation(jax.random.fold_in(own, 3), count)
    donor, receiver = mixed[0:count // 2 * 2:2], mixed[1:count // 2 * 2:2]
    slack = jnp.minimum(tallies[donor] - 1, reach - tallies[receiver]) // 2
    slack = jnp.where((donor == sequence[0]) | (receiver == sequence[0]) | (tallies[receiver] == 0), 0, jnp.maximum(slack, 0))
    shifted = jax.random.randint(jax.random.fold_in(own, 4), (count // 2,), 0, 1 << 20) % (slack + 1)
    tallies = tallies.at[donor].add(-shifted).at[receiver].add(shifted)
    labels = jnp.searchsorted(jnp.cumsum(tallies), jnp.arange(rows * top), side="right").astype(jnp.int32)
    table = labels.reshape(top, rows).T
    table = table[jax.random.permutation(jax.random.fold_in(own, 1), rows)]
    rotation = jax.random.randint(jax.random.fold_in(own, 2), (rows, 1), 0, top)
    return jnp.take_along_axis(table, (jnp.arange(top)[None, :] + rotation) % top, axis=1)


def load_shares(number_of, total, limit, skew, full):
    loads = [(1 << 20) // math.isqrt(standing ** skew) + 1 for standing in range(1, number_of + 1)]
    largest = limit if full else min(limit, max(-(-total // number_of), total * loads[0] // sum(loads)))
    least = 1 if total - largest >= number_of - 1 else 0
    counts, spare = [largest] + [least] * (number_of - 1), total - largest - least * (number_of - 1)
    while spare > 0:
        candidates = [i for i in range(1, number_of) if counts[i] < largest] or [i for i in range(1, number_of) if counts[i] < limit]
        pool, budget = sum([loads[i] for i in candidates]), spare
        for i in candidates:
            addition = min(limit - counts[i], max(1, budget * loads[i] // pool), spare)
            counts[i] = counts[i] + addition
            spare = spare - addition
    return np.array(counts)


def centred(own_key, extent, deviation, limit, cuts=(), held_as=jnp.bfloat16):
    drawn = deviation * jax.random.normal(own_key, extent, jnp.float32)
    if cuts:
        drawn = drawn * levels(own_key, extent, cuts, -0.22, 0.18)
    return jnp.clip(drawn, -limit, limit).astype(held_as)


def setup_inputs(seed: int = 0) -> dict:
    key_list = jax.random.split(jax.random.key(seed), 11)
    tokens = draw_tokens(jax.random.fold_in(key_list[10], 71), 0)
    pre_gain = jnp.clip(1.0 + 0.18 * jax.random.normal(key_list[1], (D,), jnp.float32), 0.1, 1.9)
    post_gain = jnp.clip(1.0 + 0.18 * jax.random.normal(key_list[2], (D,), jnp.float32), 0.1, 1.9)
    group_logits = centred(key_list[3], (TOKENS, GROUPS), 2.0, 12.0, ((0, 16),), jnp.float32)
    expert_logits = draw_expert_logits(jax.random.fold_in(key_list[10], 71), 0)
    route_group_keys = jax.random.split(jax.random.fold_in(key_list[5], 1), TOKENS // TOK_DEV)
    route_group_turns = jax.random.permutation(jax.random.fold_in(key_list[5], 3), TOKENS // TOK_DEV)
    route_group = jax.vmap(lambda own, number: routed_block(jax.random.fold_in(key_list[5], 2), own, number, TOK_DEV, GROUPS, TOPK, CAP, 2))(route_group_keys, route_group_turns).reshape((TOKENS, TOPK))
    route_expert = with_ends(jax.random.randint(key_list[6], (TOKENS, TOPK), 0, EXP_DEV), jax.random.fold_in(key_list[6], 1), 0, EXP_DEV - 1).astype(jnp.int32)
    gate_weight = centred(key_list[7], (EXPERTS, D, FF), D ** -0.5, 0.125, ((0, 16), (1, 2)))
    up_weight = centred(key_list[8], (EXPERTS, D, FF), D ** -0.5, 0.125, ((0, 16), (1, 2)))
    down_weight = draw_down_weight(jax.random.fold_in(key_list[10], 71), 0)
    return dict(tokens=tokens, pre_gain=pre_gain, post_gain=post_gain, group_logits=group_logits, expert_logits=expert_logits, route_group=route_group, route_expert=route_expert, gate_weight=gate_weight, up_weight=up_weight, down_weight=down_weight)


epsilon = 1e-06

def reference(tokens, pre_gain, post_gain, group_logits, expert_logits, route_group, route_expert, gate_weight, up_weight, down_weight):
    values = tokens.astype(jnp.float32)
    normed = (values * lax.rsqrt(lax.optimization_barrier(jnp.mean(values * values, axis=1, keepdims=True)) + epsilon) * pre_gain.astype(jnp.float32)).astype(jnp.bfloat16)
    picked = jnp.take_along_axis(group_logits, route_group, axis=1)
    gates = jax.nn.softmax(picked + expert_logits, axis=-1)
    expert = (route_group * EXP_DEV + route_expert).astype(jnp.int32).reshape(-1)
    repeated = jnp.repeat(normed, TOPK, axis=0)
    block = D // N_TP

    def blockwise(row, weight):
        left = row.reshape(N_TP, block).astype(jnp.float32)
        right = weight.reshape(N_TP, block, FF).astype(jnp.float32)
        parts = jnp.einsum('bd,bdf->bf', left, right).astype(jnp.bfloat16)
        return lax.optimization_barrier(jnp.sum(parts.astype(jnp.float32), axis=0))[None, :]

    def serve(entry):
        row, index = entry
        pre_gate = blockwise(row, gate_weight[index])
        pre_up = blockwise(row, up_weight[index])
        hidden = (jax.nn.silu(pre_gate) * pre_up).astype(jnp.bfloat16)
        return jnp.dot(hidden, down_weight[index], preferred_element_type=jnp.float32).astype(jnp.bfloat16)[0]
    answer = lax.map(serve, (repeated, expert)).reshape(TOKENS, TOPK, D)
    mixed = lax.optimization_barrier(jnp.sum(gates[:, :, None] * answer.astype(jnp.float32), axis=1))
    result = mixed * lax.rsqrt(lax.optimization_barrier(jnp.mean(mixed * mixed, axis=1, keepdims=True)) + epsilon) * post_gain.astype(jnp.float32)
    return result.astype(jnp.bfloat16)
```

```python
import functools

import jax
import jax.numpy as jnp
from jax import lax
from jax.experimental import pallas as pl
from jax.experimental.pallas import tpu as pltpu
from jax.sharding import PartitionSpec as P

EPS = 1e-06
MESH = pl.DeviceIdType.MESH
F32 = jnp.float32
BF16 = jnp.bfloat16
LANES = 128


def dot(a, b):
    return jnp.dot(a, b, preferred_element_type=F32)


def kernel(
    sizes,
    tok_ref, pre_ref, post_ref, glog_ref, elog_ref, rgrp_ref, rexp_ref,
    gate_hbm, up_hbm, down_hbm,
    out_ref,
    w_for, w_own, d_own, d_for,
    sq_mine, sq_peer, xg, xs, sel, acc, p_send, p_recv, h_own, h_for, spread, ans,
    part, r_core, s_x, r_x, s_z, r_z, fin, t_mine, t_peer,
    w_sem, tp_send, tp_recv, z_send, z_recv, x_send, x_recv, c_send, c_recv,
    rc_send, rc_recv, rx_send, rx_recv, rz_send, rz_recv,
):
    nz, groups, cap, top, full = sizes
    tok, width = tok_ref.shape
    experts = gate_hbm.shape[0]
    ff = gate_hbm.shape[2]
    half = ff // 2
    meta = xg.shape[3] - width
    slots = xs.shape[0]
    me = lax.axis_index("ep")
    tp = lax.axis_index("tp")
    z, x, c = me // 4, lax.rem(me // 2, 2), lax.rem(me, 2)
    q = 2 * c + x
    peer = {"ep": me, "tp": 1 - tp}
    x_peer = {"ep": z * 4 + (1 - x) * 2 + c, "tp": tp}
    c_peer = {"ep": z * 4 + x * 2 + (1 - c), "tp": tp}

    def z_peer(step):
        return {"ep": lax.rem(z + step, nz) * 4 + x * 2 + c, "tp": tp}

    own_cols = pl.ds(pl.multiple_of(tp * half, half), half)
    for_cols = pl.ds(pl.multiple_of((1 - tp) * half, half), half)
    lo, hi = pl.ds(0, half), pl.ds(half, half)
    loads = [
        pltpu.make_async_copy(src, dst, w_sem.at[i])
        for i, (src, dst) in enumerate(
            (
                (gate_hbm.at[:, :, for_cols], w_for.at[:, :, lo]),
                (up_hbm.at[:, :, for_cols], w_for.at[:, :, hi]),
                (gate_hbm.at[:, :, own_cols], w_own.at[:, :, lo]),
                (up_hbm.at[:, :, own_cols], w_own.at[:, :, hi]),
                (down_hbm.at[:, own_cols, :], d_own),
                (down_hbm.at[:, for_cols, :], d_for),
            )
        )
    ]
    for load in loads:
        load.start()

    barrier = pltpu.get_barrier_semaphore()
    for other in [peer, x_peer, c_peer] + [z_peer(s) for s in range(1, nz)]:
        pl.semaphore_signal(barrier, inc=1, device_id=other, device_id_type=MESH)

    def remote(src, dst, send, recv, target):
        return pltpu.make_async_remote_copy(
            src_ref=src, dst_ref=dst, send_sem=send, recv_sem=recv,
            device_id=target, device_id_type=MESH,
        )

    values = tok_ref[...].astype(F32)
    squares = jnp.sum(values * values, axis=1, keepdims=True)
    sq_mine[...] = jnp.broadcast_to(squares, sq_mine.shape)
    pl.semaphore_wait(barrier, nz + 2)
    sq_copy = remote(sq_mine, sq_peer, tp_send.at[0], tp_recv.at[0], peer)
    sq_copy.start()

    lane = lax.broadcasted_iota(jnp.int32, (tok, meta), 1)
    glane = lax.broadcasted_iota(jnp.int32, (tok, groups), 1)
    logits = glog_ref[...]
    scores, chosen = [], []
    for k in range(top):
        grp = rgrp_ref[:, k : k + 1]
        chosen.append(grp)
        picked = jnp.sum(jnp.where(glane == grp, logits, 0.0), axis=1, keepdims=True)
        scores.append(picked + elog_ref[:, k : k + 1])
    best = functools.reduce(jnp.maximum, scores)
    raised = [jnp.exp(s - best) for s in scores]
    total = functools.reduce(jnp.add, raised)
    info = jnp.zeros((tok, meta), F32)
    member = jnp.zeros((tok, meta), F32)
    for k in range(top):
        ids = rexp_ref[:, k : k + 1].astype(F32) + 1.0
        info = info + jnp.where(lane == chosen[k], ids, 0.0)
        info = info + jnp.where(lane == chosen[k] + 2 * groups, raised[k] / total, 0.0)
        member = member + jnp.where(lane == chosen[k] + groups, 1.0, 0.0)
    below = (
        lax.broadcasted_iota(jnp.int32, (tok, tok), 0)
        > lax.broadcasted_iota(jnp.int32, (tok, tok), 1)
    ).astype(F32)
    info = info + member * dot(below.astype(BF16), member.astype(BF16))
    xg[z, q, :, width:] = info.astype(BF16)

    sq_copy.wait()
    squares = sq_mine[:, 0:1] + sq_peer[:, 0:1]
    xg[z, q, :, :width] = (
        values * lax.rsqrt(squares / full + EPS) * pre_ref[...]
    ).astype(BF16)

    order = sorted(range(1, nz), key=lambda s: -min(s, nz - s))
    z_copies = {
        s: remote(xg.at[z, q], xg.at[z, q], z_send.at[s], z_recv.at[s], z_peer(s))
        for s in order
    }
    for s in order:
        z_copies[s].start()
    q_x = 2 * c + (1 - x)
    x_copies, c_copies = [], []
    for s in [0] + sorted(range(1, nz), key=lambda s: min(s, nz - s)):
        zs = lax.rem(z + nz - s, nz)
        if s:
            z_copies[s].wait_recv()
        block = xg.at[zs, q]
        xc = remote(block, block, x_send.at[s], x_recv.at[s], x_peer)
        xc.start()
        cc = remote(block, block, c_send.at[s, 0], c_recv.at[s, 0], c_peer)
        cc.start()
        x_copies.append((s, xc))
        c_copies.append(cc)
    for s, xc in x_copies:
        zs = lax.rem(z + nz - s, nz)
        xc.wait_recv()
        block = xg.at[zs, q_x]
        cc = remote(block, block, c_send.at[s, 1], c_recv.at[s, 1], c_peer)
        cc.start()
        c_copies.append(cc)
    for cc in c_copies:
        cc.wait()
    for s, xc in x_copies:
        xc.wait_send()
    for s in order:
        z_copies[s].wait_send()

    zt, zc = 4 * tok, 4 * cap

    def slot_of(block, place):
        return block * cap + place

    def pick(i, carry):
        rows = xg[i].reshape(zt, width + meta)
        codes = rows[:, width:]
        srow = lax.broadcasted_iota(jnp.int32, (16, meta), 0)
        slane = lax.broadcasted_iota(jnp.int32, (16, meta), 1)
        take = ((slane == me + srow * groups) & (srow < 3)).astype(F32).astype(BF16)
        picked = lax.dot_general(
            take, codes, (((1,), (1,)), ((), ())), preferred_element_type=F32
        )
        ids, place = picked[0:1, :], picked[1:2, :]
        tcol = lax.broadcasted_iota(jnp.int32, (zc, zt), 1)
        trow = lax.broadcasted_iota(jnp.int32, (zc, zt), 0)
        block = functools.reduce(
            jnp.add, [(tcol >= b * tok).astype(F32) for b in range(1, 4)]
        )
        hot = (trow.astype(F32) == block * cap + place) & (ids > 0.5)
        at = pl.ds(pl.multiple_of(i * zc, 16), zc)
        xs[at, :] = dot(hot.astype(F32).astype(BF16), rows[:, :width]).astype(BF16)
        sel[at, :] = jnp.broadcast_to(
            jnp.sum(jnp.where(hot, ids, 0.0), axis=1, keepdims=True), (zc, LANES)
        )
        return carry

    lax.fori_loop(0, nz, pick, 0)

    def project(weights):
        acc[...] = jnp.zeros_like(acc)

        def step(e, carry):
            on = (sel[...] == (e + 1).astype(F32)).astype(F32).astype(BF16)
            on = jnp.concatenate([on] * (width // LANES), axis=1)
            acc[...] += dot(xs[...] * on, weights[e])
            return carry

        lax.fori_loop(0, experts, step, 0)

    loads[0].wait()
    loads[1].wait()
    project(w_for)
    p_send[...] = acc[...].astype(BF16)
    p_copy = remote(p_send, p_recv, tp_send.at[1], tp_recv.at[1], peer)
    p_copy.start()
    loads[2].wait()
    loads[3].wait()
    project(w_own)
    p_copy.wait()
    pre = acc[...].astype(BF16).astype(F32) + p_recv[...].astype(F32)
    g, u = pre[:, :half], pre[:, half:]
    h_own[...] = (g / (1.0 + jnp.exp(-g)) * u).astype(BF16)
    h_copy = remote(h_own, h_for, tp_send.at[2], tp_recv.at[2], peer)
    h_copy.start()

    tile = 256 if width % 256 == 0 else LANES

    def down(hidden, weights, first):
        for e in range(experts):
            on = (sel[...] == float(e + 1)).astype(F32).astype(BF16)
            if half != LANES:
                on = jnp.concatenate([on] * (half // LANES), axis=1)
            spread[:, e * half : (e + 1) * half] = hidden[...] * on

        def step(j, carry):
            at = pl.ds(pl.multiple_of(j * tile, tile), tile)
            w = weights[:, :, at].reshape(experts * half, tile)
            got = dot(spread[...], w)
            ans[:, at] = got if first else ans[:, at] + got
            return carry

        lax.fori_loop(0, width // tile, step, 0)

    loads[4].wait()
    down(h_own, d_own, True)
    loads[5].wait()
    h_copy.wait()
    down(h_for, d_for, False)

    def combine(i, carry):
        codes = xg[i, :, :, width:].reshape(zt, meta).astype(F32)
        clane = lax.broadcasted_iota(jnp.int32, (zt, meta), 1)

        def column(j):
            return jnp.sum(
                jnp.where(clane == me + j * groups, codes, 0.0), axis=1, keepdims=True
            )

        ids, place, gate = column(0), column(1), column(2)
        trow = lax.broadcasted_iota(jnp.int32, (zt, zc), 0)
        tcol = lax.broadcasted_iota(jnp.int32, (zt, zc), 1).astype(F32)
        block = functools.reduce(
            jnp.add, [(trow >= b * tok).astype(F32) for b in range(1, 4)]
        )
        hot = (tcol == block * cap + place) & (ids > 0.5)
        mix = jnp.where(hot, gate, 0.0).astype(BF16)
        at = pl.ds(pl.multiple_of(i * zc, 16), zc)
        got = dot(mix, ans[at, :].astype(BF16))
        part[i] = got.astype(BF16).reshape(4, tok, width)
        return carry

    lax.fori_loop(0, nz, combine, 0)

    far = order + [0]
    core_copies = {}
    for s in far:
        zs = lax.rem(z + s, nz)
        core_copies[s] = remote(
            part.at[zs, pl.ds(2 * (1 - c), 2)], r_core.at[zs],
            rc_send.at[s], rc_recv.at[s], c_peer,
        )
        core_copies[s].start()
    rx_copies = {}
    for s in far:
        zs = lax.rem(z + s, nz)
        core_copies[s].wait_recv()
        s_x[zs] = (
            part[zs, 2 * c + (1 - x)].astype(F32) + r_core[zs, 1 - x].astype(F32)
        ).astype(BF16)
        rx_copies[s] = remote(s_x.at[zs], r_x.at[zs], rx_send.at[s], rx_recv.at[s], x_peer)
        rx_copies[s].start()
    rz_copies = {}
    for s in far:
        zs = lax.rem(z + s, nz)
        rx_copies[s].wait_recv()
        summed = (
            part[zs, q].astype(F32) + r_core[zs, x].astype(F32) + r_x[zs].astype(F32)
        )
        if s:
            s_z[s] = summed.astype(BF16)
            rz_copies[s] = remote(
                s_z.at[s], r_z.at[s], rz_send.at[s], rz_recv.at[s], z_peer(s)
            )
            rz_copies[s].start()
        else:
            fin[...] = summed
    mixed = fin[...]
    for s in order:
        rz_copies[s].wait_recv()
        mixed = mixed + r_z[s].astype(F32)
    fin[...] = mixed
    t_mine[...] = jnp.broadcast_to(
        jnp.sum(mixed * mixed, axis=1, keepdims=True), t_mine.shape
    )
    t_copy = remote(t_mine, t_peer, tp_send.at[3], tp_recv.at[3], peer)
    t_copy.start()
    for s in far:
        core_copies[s].wait_send()
        rx_copies[s].wait_send()
        if s:
            rz_copies[s].wait_send()
    t_copy.wait()
    totals = t_mine[:, 0:1] + t_peer[:, 0:1]
    out_ref[...] = (
        fin[...] * lax.rsqrt(totals / full + EPS) * post_ref[...]
    ).astype(BF16)


def expert_rows(rows, indices, gate_weight, up_weight, down_weight):
    experts_here = gate_weight.shape[0]
    chosen_hot = indices[None, :] == jnp.arange(experts_here, dtype=jnp.int32)[:, None]
    chosen = jnp.where(chosen_hot[:, :, None], rows[None, :, :], jnp.zeros((), jnp.bfloat16))
    part_gate = jnp.einsum(
        "esd,edf->sf", chosen, gate_weight, preferred_element_type=jnp.float32
    ).astype(jnp.bfloat16)
    part_up = jnp.einsum(
        "esd,edf->sf", chosen, up_weight, preferred_element_type=jnp.float32
    ).astype(jnp.bfloat16)
    share_gate, share_up = (
        lax.psum_scatter(part_gate, "tp", scatter_dimension=1, tiled=True).astype(jnp.float32),
        lax.psum_scatter(part_up, "tp", scatter_dimension=1, tiled=True).astype(jnp.float32),
    )
    share_hidden = (jax.nn.silu(share_gate) * share_up).astype(jnp.bfloat16)
    hidden = lax.all_gather(share_hidden, "tp", axis=1, tiled=True)
    spread = jnp.where(chosen_hot[:, :, None], hidden[None, :, :], jnp.zeros((), jnp.bfloat16))
    return jnp.einsum(
        "esf,efd->sd", spread, down_weight, preferred_element_type=jnp.float32
    ).astype(jnp.bfloat16)


def any_mesh(
    tokens,
    pre_gain,
    post_gain,
    group_logits,
    expert_logits,
    route_group,
    route_expert,
    gate_weight,
    up_weight,
    down_weight,
):
    tok_count, local_width = tokens.shape
    top_count = route_group.shape[1]
    group_count = lax.axis_size("ep")
    full_width = local_width * lax.axis_size("tp")
    capacity = min(
        tok_count, max(2, (3 * tok_count * top_count + 2 * group_count - 1) // (2 * group_count))
    )
    slot_count = group_count * capacity
    values = tokens.astype(jnp.float32)
    squares = lax.psum(jnp.sum(values * values, axis=1), "tp")
    normed = (values * lax.rsqrt(squares / full_width + EPS)[:, None] * pre_gain).astype(
        jnp.bfloat16
    )
    group_table = route_group[:, :, None] == jnp.arange(group_count, dtype=jnp.int32)[None, None, :]
    picked = jnp.sum(jnp.where(group_table, group_logits[:, None, :], 0.0), axis=2)
    gates = jax.nn.softmax(picked + expert_logits, axis=-1)
    flat_group = route_group.reshape(-1)
    flat_expert = route_expert.reshape(-1)
    group_hot = (flat_group[:, None] == jnp.arange(group_count, dtype=jnp.int32)[None, :]).astype(
        jnp.int32
    )
    earlier = jnp.cumsum(group_hot, axis=0) - group_hot
    within = jnp.sum(earlier * group_hot, axis=1)
    slot_index = flat_group * capacity + within
    slot_hot = slot_index[:, None] == jnp.arange(slot_count, dtype=jnp.int32)[None, :]
    placed = slot_hot.reshape(tok_count, top_count, slot_count)
    picker = jnp.any(placed, axis=1).astype(jnp.bfloat16)
    send_rows = jnp.einsum("ts,td->sd", picker, normed, preferred_element_type=jnp.float32).astype(
        jnp.bfloat16
    )
    send_ids = jnp.sum(jnp.where(slot_hot, flat_expert[:, None] + 1, 0), axis=0) - 1
    rows = lax.all_to_all(
        send_rows.reshape(group_count, capacity, local_width),
        "ep",
        split_axis=0,
        concat_axis=0,
        tiled=True,
    )
    indices = lax.all_to_all(
        send_ids.reshape(group_count, capacity), "ep", split_axis=0, concat_axis=0, tiled=True
    )
    groups_in, items = indices.shape
    served = expert_rows(
        rows.reshape(groups_in * items, local_width),
        indices.reshape(-1),
        gate_weight,
        up_weight,
        down_weight,
    )
    answered = served.reshape(groups_in, items, local_width)
    returned = lax.all_to_all(answered, "ep", split_axis=0, concat_axis=0, tiled=True)
    weights = jnp.sum(placed.astype(jnp.float32) * gates[:, :, None], axis=1)
    mixed = jnp.dot(
        weights,
        returned.reshape(slot_count, local_width).astype(jnp.float32),
        precision=lax.Precision.HIGHEST,
    )
    totals = lax.psum(jnp.sum(mixed * mixed, axis=1), "tp")
    result = mixed * lax.rsqrt(totals / full_width + EPS)[:, None] * post_gain
    return result.astype(jnp.bfloat16)


def on_device(
    tokens, pre_gain, post_gain, group_logits, expert_logits, route_group, route_expert,
    gate_weight, up_weight, down_weight,
):
    tok, width = tokens.shape
    top = route_group.shape[1]
    groups = lax.axis_size("ep")
    if lax.axis_size("tp") != 2 or groups % 4 or width % LANES or gate_weight.shape[2] % 256:
        return any_mesh(
            tokens, pre_gain, post_gain, group_logits, expert_logits, route_group,
            route_expert, gate_weight, up_weight, down_weight,
        )
    nz = groups // 4
    full = width * lax.axis_size("tp")
    cap = min(tok, max(2, (3 * tok * top + 2 * groups - 1) // (2 * groups)))
    cap = (4 * cap + 15) // 16 * 4
    slots = groups * cap
    experts, _, ff = gate_weight.shape
    half = ff // 2
    meta = (3 * groups + LANES - 1) // LANES * LANES
    vmem = pl.BlockSpec(memory_space=pltpu.VMEM)
    hbm = pl.BlockSpec(memory_space=pl.ANY)
    dma = pltpu.SemaphoreType.DMA
    scratch = [
        pltpu.VMEM((experts, width, ff), BF16),
        pltpu.VMEM((experts, width, ff), BF16),
        pltpu.VMEM((experts, half, width), BF16),
        pltpu.VMEM((experts, half, width), BF16),
        pltpu.VMEM((tok, LANES), F32),
        pltpu.VMEM((tok, LANES), F32),
        pltpu.VMEM((nz, 4, tok, width + meta), BF16),
        pltpu.VMEM((slots, width), BF16),
        pltpu.VMEM((slots, LANES), F32),
        pltpu.VMEM((slots, ff), F32),
        pltpu.VMEM((slots, ff), BF16),
        pltpu.VMEM((slots, ff), BF16),
        pltpu.VMEM((slots, half), BF16),
        pltpu.VMEM((slots, half), BF16),
        pltpu.VMEM((slots, experts * half), BF16),
        pltpu.VMEM((slots, width), F32),
        pltpu.VMEM((nz, 4, tok, width), BF16),
        pltpu.VMEM((nz, 2, tok, width), BF16),
        pltpu.VMEM((nz, tok, width), BF16),
        pltpu.VMEM((nz, tok, width), BF16),
        pltpu.VMEM((nz, tok, width), BF16),
        pltpu.VMEM((nz, tok, width), BF16),
        pltpu.VMEM((tok, width), F32),
        pltpu.VMEM((tok, LANES), F32),
        pltpu.VMEM((tok, LANES), F32),
        dma((6,)), dma((4,)), dma((4,)),
        dma((nz,)), dma((nz,)), dma((nz,)), dma((nz,)), dma((nz, 2)), dma((nz, 2)),
        dma((nz,)), dma((nz,)), dma((nz,)), dma((nz,)), dma((nz,)), dma((nz,)),
    ]
    return pl.pallas_call(
        functools.partial(kernel, (nz, groups, cap, top, full)),
        out_shape=jax.ShapeDtypeStruct((tok, width), BF16),
        in_specs=[vmem] * 7 + [hbm] * 3,
        out_specs=vmem,
        scratch_shapes=scratch,
        compiler_params=pltpu.CompilerParams(
            collective_id=0, has_side_effects=True, vmem_limit_bytes=63 * 1024 * 1024
        ),
    )(
        tokens, pre_gain.reshape(1, width), post_gain.reshape(1, width), group_logits,
        expert_logits, route_group, route_expert, gate_weight, up_weight, down_weight,
    )


def solution(mesh):
    in_specs = (
        P("ep", "tp"), P("tp"), P("tp"), P("ep", None), P("ep", None), P("ep", None),
        P("ep", None), P("ep", "tp", None), P("ep", "tp", None), P("ep", None, "tp"),
    )
    return jax.shard_map(
        on_device, mesh=mesh, in_specs=in_specs, out_specs=P("ep", "tp"), check_vma=False
    )
```

```python
import functools

import jax
import jax.numpy as jnp
from jax import lax
from jax.experimental import pallas as pl
from jax.experimental.pallas import tpu as pltpu
from jax.sharding import PartitionSpec as P

EPS = 1e-06
MESH = pl.DeviceIdType.MESH
F32 = jnp.float32
BF16 = jnp.bfloat16
LANES = 128


def dot(a, b):
    return jnp.dot(a, b, preferred_element_type=F32)


def kernel(
    sizes,
    tok_ref, pre_ref, post_ref, glog_ref, elog_ref, rgrp_ref, rexp_ref,
    gate_hbm, up_hbm, down_hbm,
    out_ref,
    w_for, w_own, d_own, d_for,
    sq_mine, sq_peer, xg, xs, sel, own, p_send, p_recv, h_own, h_for, spread, ans,
    part, r_core, s_x, r_x, s_z, r_z, fin, t_mine, t_peer,
    w_sem, tp_send, tp_recv, z_send, z_recv, x_send, x_recv, c_send, c_recv,
    rc_send, rc_recv, rx_send, rx_recv, rz_send, rz_recv,
):
    nz, groups, cap, top, full = sizes
    tok, width = tok_ref.shape
    experts = gate_hbm.shape[0]
    ff = gate_hbm.shape[2]
    half = ff // 2
    meta = xg.shape[3] - width
    slots = xs.shape[0]
    me = lax.axis_index("ep")
    tp = lax.axis_index("tp")
    z, x, c = me // 4, lax.rem(me // 2, 2), lax.rem(me, 2)
    q = 2 * c + x
    peer = {"ep": me, "tp": 1 - tp}
    x_peer = {"ep": z * 4 + (1 - x) * 2 + c, "tp": tp}
    c_peer = {"ep": z * 4 + x * 2 + (1 - c), "tp": tp}

    def z_peer(step):
        return {"ep": lax.rem(z + step, nz) * 4 + x * 2 + c, "tp": tp}

    own_cols = pl.ds(pl.multiple_of(tp * half, half), half)
    for_cols = pl.ds(pl.multiple_of((1 - tp) * half, half), half)
    lo, hi = pl.ds(0, half), pl.ds(half, half)
    loads = [
        pltpu.make_async_copy(src, dst, w_sem.at[i])
        for i, (src, dst) in enumerate(
            (
                (gate_hbm.at[:, :, for_cols], w_for.at[:, :, lo]),
                (up_hbm.at[:, :, for_cols], w_for.at[:, :, hi]),
                (gate_hbm.at[:, :, own_cols], w_own.at[:, :, lo]),
                (up_hbm.at[:, :, own_cols], w_own.at[:, :, hi]),
                (down_hbm.at[:, own_cols, :], d_own),
                (down_hbm.at[:, for_cols, :], d_for),
            )
        )
    ]
    for load in loads:
        load.start()

    barrier = pltpu.get_barrier_semaphore()
    for other in [peer, x_peer, c_peer] + [z_peer(s) for s in range(1, nz)]:
        pl.semaphore_signal(barrier, inc=1, device_id=other, device_id_type=MESH)

    def remote(src, dst, send, recv, target):
        return pltpu.make_async_remote_copy(
            src_ref=src, dst_ref=dst, send_sem=send, recv_sem=recv,
            device_id=target, device_id_type=MESH,
        )

    values = tok_ref[...].astype(F32)
    squares = jnp.sum(values * values, axis=1, keepdims=True)
    sq_mine[...] = jnp.broadcast_to(squares, sq_mine.shape)
    pl.semaphore_wait(barrier, nz + 2)
    sq_copy = remote(sq_mine, sq_peer, tp_send.at[0], tp_recv.at[0], peer)
    sq_copy.start()

    lane = lax.broadcasted_iota(jnp.int32, (tok, meta), 1)
    glane = lax.broadcasted_iota(jnp.int32, (tok, groups), 1)
    logits = glog_ref[...]
    scores, chosen = [], []
    for k in range(top):
        grp = rgrp_ref[:, k : k + 1]
        chosen.append(grp)
        picked = jnp.sum(jnp.where(glane == grp, logits, 0.0), axis=1, keepdims=True)
        scores.append(picked + elog_ref[:, k : k + 1])
    best = functools.reduce(jnp.maximum, scores)
    raised = [jnp.exp(s - best) for s in scores]
    total = functools.reduce(jnp.add, raised)
    info = jnp.zeros((tok, meta), F32)
    member = jnp.zeros((tok, meta), F32)
    for k in range(top):
        ids = rexp_ref[:, k : k + 1].astype(F32) + 1.0
        info = info + jnp.where(lane == chosen[k], ids, 0.0)
        info = info + jnp.where(lane == chosen[k] + 2 * groups, raised[k] / total, 0.0)
        member = member + jnp.where(lane == chosen[k] + groups, 1.0, 0.0)
    below = (
        lax.broadcasted_iota(jnp.int32, (tok, tok), 0)
        > lax.broadcasted_iota(jnp.int32, (tok, tok), 1)
    ).astype(F32)
    info = info + member * dot(below.astype(BF16), member.astype(BF16))
    xg[z, q, :, width:] = info.astype(BF16)

    sq_copy.wait()
    squares = sq_mine[:, 0:1] + sq_peer[:, 0:1]
    xg[z, q, :, :width] = (
        values * lax.rsqrt(squares / full + EPS) * pre_ref[...]
    ).astype(BF16)

    order = sorted(range(1, nz), key=lambda s: -min(s, nz - s))
    z_copies = {
        s: remote(xg.at[z, q], xg.at[z, q], z_send.at[s], z_recv.at[s], z_peer(s))
        for s in order
    }
    for s in order:
        z_copies[s].start()
    q_x = 2 * c + (1 - x)
    near = [0] + order[::-1]
    x_copies, c_copies = {}, {}

    def forward_own(s):
        if s:
            z_copies[s].wait_recv()
        block = xg.at[lax.rem(z + nz - s, nz), q]
        x_copies[s] = remote(block, block, x_send.at[s], x_recv.at[s], x_peer)
        x_copies[s].start()
        cc = remote(block, block, c_send.at[s, 0], c_recv.at[s, 0], c_peer)
        cc.start()
        c_copies[s] = [cc]

    def forward_side(s):
        x_copies[s].wait_recv()
        block = xg.at[lax.rem(z + nz - s, nz), q_x]
        cc = remote(block, block, c_send.at[s, 1], c_recv.at[s, 1], c_peer)
        cc.start()
        c_copies[s].append(cc)
        for copy in c_copies[s]:
            copy.wait_recv()

    zt, zc = 4 * tok, 4 * cap

    def pick(i):
        rows = xg[i].reshape(zt, width + meta)
        codes = rows[:, width:]
        srow = lax.broadcasted_iota(jnp.int32, (16, meta), 0)
        slane = lax.broadcasted_iota(jnp.int32, (16, meta), 1)
        take = ((slane == me + srow * groups) & (srow < 3)).astype(F32).astype(BF16)
        picked = lax.dot_general(
            take, codes, (((1,), (1,)), ((), ())), preferred_element_type=F32
        )
        ids, place = picked[0:1, :], picked[1:2, :]
        tcol = lax.broadcasted_iota(jnp.int32, (zc, zt), 1)
        trow = lax.broadcasted_iota(jnp.int32, (zc, zt), 0)
        block = functools.reduce(
            jnp.add, [(tcol >= b * tok).astype(F32) for b in range(1, 4)]
        )
        hot = (trow.astype(F32) == block * cap + place) & (ids > 0.5)
        at = pl.ds(pl.multiple_of(i * zc, 16), zc)
        xs[at, :] = dot(hot.astype(F32).astype(BF16), rows[:, :width]).astype(BF16)
        sel[at, :] = jnp.broadcast_to(
            jnp.sum(jnp.where(hot, ids, 0.0), axis=1, keepdims=True), (zc, LANES)
        )

    def project(at, weights):
        def step(e, total):
            on = (sel[at, :] == (e + 1).astype(F32)).astype(F32).astype(BF16)
            on = jnp.concatenate([on] * (width // LANES), axis=1)
            return total + dot(xs[at, :] * on, weights[e])

        return lax.fori_loop(0, experts, step, jnp.zeros((zc, ff), F32))

    p_copies, h_copies = {}, {}

    def rows_of(s):
        return pl.ds(pl.multiple_of(lax.rem(z + nz - s, nz) * zc, 16), zc)

    def finish(s):
        at = rows_of(s)
        p_copies[s].wait_recv()
        pre = own[at, :].astype(F32) + p_recv[at, :].astype(F32)
        g, u = pre[:, :half], pre[:, half:]
        h_own[at, :] = (g / (1.0 + jnp.exp(-g)) * u).astype(BF16)
        h_copies[s] = remote(
            h_own.at[at], h_for.at[at], tp_send.at[2 + nz + s], tp_recv.at[2 + nz + s], peer
        )
        h_copies[s].start()

    forward_own(near[0])
    for n, s in enumerate(near):
        if n + 1 < nz:
            forward_own(near[n + 1])
        forward_side(s)
        pick(lax.rem(z + nz - s, nz))
        at = rows_of(s)
        if n == 0:
            for load in loads[:4]:
                load.wait()
        p_send[at, :] = project(at, w_for).astype(BF16)
        p_copies[s] = remote(
            p_send.at[at], p_recv.at[at], tp_send.at[2 + s], tp_recv.at[2 + s], peer
        )
        p_copies[s].start()
        own[at, :] = project(at, w_own).astype(BF16)
        if n:
            finish(near[n - 1])
    finish(near[-1])
    for s in near:
        x_copies[s].wait_send()
        for copy in c_copies[s]:
            copy.wait_send()
        if s:
            z_copies[s].wait_send()

    tile = 256 if width % 256 == 0 else LANES

    def down(at):
        for e in range(experts):
            on = (sel[at, :] == float(e + 1)).astype(F32).astype(BF16)
            if half != LANES:
                on = jnp.concatenate([on] * (half // LANES), axis=1)
            cols = slice(e * half, (e + 1) * half)
            spread[0, :, cols] = h_own[at, :] * on
            spread[1, :, cols] = h_for[at, :] * on

        def step(j, carry):
            cols = pl.ds(pl.multiple_of(j * tile, tile), tile)
            one = dot(spread[0], d_own[:, :, cols].reshape(experts * half, tile))
            two = dot(spread[1], d_for[:, :, cols].reshape(experts * half, tile))
            ans[:, cols] = (one + two).astype(BF16)
            return carry

        lax.fori_loop(0, width // tile, step, 0)

    def combine(i):
        codes = xg[i, :, :, width:].reshape(zt, meta).astype(F32)
        clane = lax.broadcasted_iota(jnp.int32, (zt, meta), 1)

        def column(j):
            return jnp.sum(
                jnp.where(clane == me + j * groups, codes, 0.0), axis=1, keepdims=True
            )

        ids, place, gate = column(0), column(1), column(2)
        trow = lax.broadcasted_iota(jnp.int32, (zt, zc), 0)
        tcol = lax.broadcasted_iota(jnp.int32, (zt, zc), 1).astype(F32)
        block = functools.reduce(
            jnp.add, [(trow >= b * tok).astype(F32) for b in range(1, 4)]
        )
        hot = (tcol == block * cap + place) & (ids > 0.5)
        mix = jnp.where(hot, gate, 0.0).astype(BF16)
        part[i] = dot(mix, ans[...]).astype(BF16).reshape(4, tok, width)

    loads[4].wait()
    loads[5].wait()
    core_copies, rx_copies = {}, {}

    def send_side(s):
        zs = lax.rem(z + s, nz)
        core_copies[s].wait_recv()
        s_x[zs] = (
            part[zs, 2 * c + (1 - x)].astype(F32) + r_core[zs, 1 - x].astype(F32)
        ).astype(BF16)
        rx_copies[s] = remote(s_x.at[zs], r_x.at[zs], rx_send.at[s], rx_recv.at[s], x_peer)
        rx_copies[s].start()

    back = near[1:] + [0]
    for s in back:
        zs = lax.rem(z + nz - s, nz)
        h_copies[s].wait_recv()
        down(rows_of(s))
        combine(zs)
        core_copies[nz - s if s else 0] = copy = remote(
            part.at[zs, pl.ds(2 * (1 - c), 2)], r_core.at[zs],
            rc_send.at[s], rc_recv.at[s], c_peer,
        )
        copy.start()
        if s != back[0]:
            send_side(last)
        last = nz - s if s else 0
    send_side(last)
    far = list(rx_copies)
    rz_copies = {}
    for s in far:
        zs = lax.rem(z + s, nz)
        rx_copies[s].wait_recv()
        summed = (
            part[zs, q].astype(F32) + r_core[zs, x].astype(F32) + r_x[zs].astype(F32)
        )
        if s:
            s_z[s] = summed.astype(BF16)
            rz_copies[s] = remote(
                s_z.at[s], r_z.at[s], rz_send.at[s], rz_recv.at[s], z_peer(s)
            )
            rz_copies[s].start()
        else:
            fin[...] = summed
    mixed = fin[...]
    for s in order:
        rz_copies[s].wait_recv()
        mixed = mixed + r_z[s].astype(F32)
    fin[...] = mixed
    t_mine[...] = jnp.broadcast_to(
        jnp.sum(mixed * mixed, axis=1, keepdims=True), t_mine.shape
    )
    t_copy = remote(t_mine, t_peer, tp_send.at[1], tp_recv.at[1], peer)
    t_copy.start()
    for s in near:
        p_copies[s].wait_send()
        h_copies[s].wait_send()
    for s in far:
        core_copies[s].wait_send()
        rx_copies[s].wait_send()
        if s:
            rz_copies[s].wait_send()
    t_copy.wait()
    totals = t_mine[:, 0:1] + t_peer[:, 0:1]
    out_ref[...] = (
        fin[...] * lax.rsqrt(totals / full + EPS) * post_ref[...]
    ).astype(BF16)


def expert_rows(rows, indices, gate_weight, up_weight, down_weight):
    experts_here = gate_weight.shape[0]
    chosen_hot = indices[None, :] == jnp.arange(experts_here, dtype=jnp.int32)[:, None]
    chosen = jnp.where(chosen_hot[:, :, None], rows[None, :, :], jnp.zeros((), jnp.bfloat16))
    part_gate = jnp.einsum(
        "esd,edf->sf", chosen, gate_weight, preferred_element_type=jnp.float32
    ).astype(jnp.bfloat16)
    part_up = jnp.einsum(
        "esd,edf->sf", chosen, up_weight, preferred_element_type=jnp.float32
    ).astype(jnp.bfloat16)
    share_gate, share_up = (
        lax.psum_scatter(part_gate, "tp", scatter_dimension=1, tiled=True).astype(jnp.float32),
        lax.psum_scatter(part_up, "tp", scatter_dimension=1, tiled=True).astype(jnp.float32),
    )
    share_hidden = (jax.nn.silu(share_gate) * share_up).astype(jnp.bfloat16)
    hidden = lax.all_gather(share_hidden, "tp", axis=1, tiled=True)
    spread = jnp.where(chosen_hot[:, :, None], hidden[None, :, :], jnp.zeros((), jnp.bfloat16))
    return jnp.einsum(
        "esf,efd->sd", spread, down_weight, preferred_element_type=jnp.float32
    ).astype(jnp.bfloat16)


def any_mesh(
    tokens,
    pre_gain,
    post_gain,
    group_logits,
    expert_logits,
    route_group,
    route_expert,
    gate_weight,
    up_weight,
    down_weight,
):
    tok_count, local_width = tokens.shape
    top_count = route_group.shape[1]
    group_count = lax.axis_size("ep")
    full_width = local_width * lax.axis_size("tp")
    capacity = min(
        tok_count, max(2, (3 * tok_count * top_count + 2 * group_count - 1) // (2 * group_count))
    )
    slot_count = group_count * capacity
    values = tokens.astype(jnp.float32)
    squares = lax.psum(jnp.sum(values * values, axis=1), "tp")
    normed = (values * lax.rsqrt(squares / full_width + EPS)[:, None] * pre_gain).astype(
        jnp.bfloat16
    )
    group_table = route_group[:, :, None] == jnp.arange(group_count, dtype=jnp.int32)[None, None, :]
    picked = jnp.sum(jnp.where(group_table, group_logits[:, None, :], 0.0), axis=2)
    gates = jax.nn.softmax(picked + expert_logits, axis=-1)
    flat_group = route_group.reshape(-1)
    flat_expert = route_expert.reshape(-1)
    group_hot = (flat_group[:, None] == jnp.arange(group_count, dtype=jnp.int32)[None, :]).astype(
        jnp.int32
    )
    earlier = jnp.cumsum(group_hot, axis=0) - group_hot
    within = jnp.sum(earlier * group_hot, axis=1)
    slot_index = flat_group * capacity + within
    slot_hot = slot_index[:, None] == jnp.arange(slot_count, dtype=jnp.int32)[None, :]
    placed = slot_hot.reshape(tok_count, top_count, slot_count)
    picker = jnp.any(placed, axis=1).astype(jnp.bfloat16)
    send_rows = jnp.einsum("ts,td->sd", picker, normed, preferred_element_type=jnp.float32).astype(
        jnp.bfloat16
    )
    send_ids = jnp.sum(jnp.where(slot_hot, flat_expert[:, None] + 1, 0), axis=0) - 1
    rows = lax.all_to_all(
        send_rows.reshape(group_count, capacity, local_width),
        "ep",
        split_axis=0,
        concat_axis=0,
        tiled=True,
    )
    indices = lax.all_to_all(
        send_ids.reshape(group_count, capacity), "ep", split_axis=0, concat_axis=0, tiled=True
    )
    groups_in, items = indices.shape
    served = expert_rows(
        rows.reshape(groups_in * items, local_width),
        indices.reshape(-1),
        gate_weight,
        up_weight,
        down_weight,
    )
    answered = served.reshape(groups_in, items, local_width)
    returned = lax.all_to_all(answered, "ep", split_axis=0, concat_axis=0, tiled=True)
    weights = jnp.sum(placed.astype(jnp.float32) * gates[:, :, None], axis=1)
    mixed = jnp.dot(
        weights,
        returned.reshape(slot_count, local_width).astype(jnp.float32),
        precision=lax.Precision.HIGHEST,
    )
    totals = lax.psum(jnp.sum(mixed * mixed, axis=1), "tp")
    result = mixed * lax.rsqrt(totals / full_width + EPS)[:, None] * post_gain
    return result.astype(jnp.bfloat16)


def on_device(
    tokens, pre_gain, post_gain, group_logits, expert_logits, route_group, route_expert,
    gate_weight, up_weight, down_weight,
):
    tok, width = tokens.shape
    top = route_group.shape[1]
    groups = lax.axis_size("ep")
    if lax.axis_size("tp") != 2 or groups % 4 or width % LANES or gate_weight.shape[2] % 256:
        return any_mesh(
            tokens, pre_gain, post_gain, group_logits, expert_logits, route_group,
            route_expert, gate_weight, up_weight, down_weight,
        )
    nz = groups // 4
    full = width * lax.axis_size("tp")
    cap = min(tok, max(2, (3 * tok * top + 2 * groups - 1) // (2 * groups)))
    cap = (4 * cap + 15) // 16 * 4
    slots = groups * cap
    experts, _, ff = gate_weight.shape
    half = ff // 2
    meta = (3 * groups + LANES - 1) // LANES * LANES
    vmem = pl.BlockSpec(memory_space=pltpu.VMEM)
    hbm = pl.BlockSpec(memory_space=pl.ANY)
    dma = pltpu.SemaphoreType.DMA
    scratch = [
        pltpu.VMEM((experts, width, ff), BF16),
        pltpu.VMEM((experts, width, ff), BF16),
        pltpu.VMEM((experts, half, width), BF16),
        pltpu.VMEM((experts, half, width), BF16),
        pltpu.VMEM((tok, LANES), F32),
        pltpu.VMEM((tok, LANES), F32),
        pltpu.VMEM((nz, 4, tok, width + meta), BF16),
        pltpu.VMEM((slots, width), BF16),
        pltpu.VMEM((slots, LANES), F32),
        pltpu.VMEM((slots, ff), BF16),
        pltpu.VMEM((slots, ff), BF16),
        pltpu.VMEM((slots, ff), BF16),
        pltpu.VMEM((slots, half), BF16),
        pltpu.VMEM((slots, half), BF16),
        pltpu.VMEM((2, 4 * cap, experts * half), BF16),
        pltpu.VMEM((4 * cap, width), BF16),
        pltpu.VMEM((nz, 4, tok, width), BF16),
        pltpu.VMEM((nz, 2, tok, width), BF16),
        pltpu.VMEM((nz, tok, width), BF16),
        pltpu.VMEM((nz, tok, width), BF16),
        pltpu.VMEM((nz, tok, width), BF16),
        pltpu.VMEM((nz, tok, width), BF16),
        pltpu.VMEM((tok, width), F32),
        pltpu.VMEM((tok, LANES), F32),
        pltpu.VMEM((tok, LANES), F32),
        dma((6,)), dma((2 * nz + 2,)), dma((2 * nz + 2,)),
        dma((nz,)), dma((nz,)), dma((nz,)), dma((nz,)), dma((nz, 2)), dma((nz, 2)),
        dma((nz,)), dma((nz,)), dma((nz,)), dma((nz,)), dma((nz,)), dma((nz,)),
    ]
    return pl.pallas_call(
        functools.partial(kernel, (nz, groups, cap, top, full)),
        out_shape=jax.ShapeDtypeStruct((tok, width), BF16),
        in_specs=[vmem] * 7 + [hbm] * 3,
        out_specs=vmem,
        scratch_shapes=scratch,
        compiler_params=pltpu.CompilerParams(
            collective_id=0, has_side_effects=True, vmem_limit_bytes=63 * 1024 * 1024
        ),
    )(
        tokens, pre_gain.reshape(1, width), post_gain.reshape(1, width), group_logits,
        expert_logits, route_group, route_expert, gate_weight, up_weight, down_weight,
    )


def solution(mesh):
    in_specs = (
        P("ep", "tp"), P("tp"), P("tp"), P("ep", None), P("ep", None), P("ep", None),
        P("ep", None), P("ep", "tp", None), P("ep", "tp", None), P("ep", None, "tp"),
    )
    return jax.shard_map(
        on_device, mesh=mesh, in_specs=in_specs, out_specs=P("ep", "tp"), check_vma=False
    )
```
